32 devices in a mesh: sp: 8 (over z, x), tp: 4 (over y, core).
Axes of the slice: x: 2, y: 2, z: 4, core: 2. Of those that a mesh axis runs over, the one named last changes fastest.
Arguments:
- residual: bfloat16 [2560, 2048], P(('sp', 'tp')), may hold values from -6 to 6
- query_narrow: bfloat16 [2560, 1024], P('sp', 'tp'), may hold values from -48 to 48
- key_narrow: bfloat16 [2560, 1024], P('sp', 'tp'), may hold values from -48 to 48
- value_narrow: bfloat16 [2560, 1024], P('sp', 'tp'), may hold values from -6 to 6
- query_wide: bfloat16 [2560, 2048], P('sp', 'tp'), may hold values from -48 to 48
- key_wide: bfloat16 [2560, 2048], P('sp', 'tp'), may hold values from -48 to 48
- value_wide: bfloat16 [2560, 1024], P('sp', 'tp'), may hold values from -6 to 6
- subtract_narrow: float32 [8], P('tp'), may hold values from 0.3 to 0.8
- subtract_wide: float32 [8], P('tp'), may hold values from 0.3 to 0.8
- head_gain: float32 [128], replicated, may hold values from 0.1 to 1.9
- out_narrow: bfloat16 [1024, 2048], replicated, may hold values from -0.125 to 0.125
- out_wide: bfloat16 [1024, 2048], replicated, may hold values from -0.125 to 0.125
- norm1_gain: float32 [2048], replicated, may hold values from 0.1 to 1.9
- norm2_gain: float32 [2048], replicated, may hold values from 0.1 to 1.9
- expert_ids: int32 [2560, 2], P(('sp', 'tp')), may hold values from 0 to 7, all different within a row; in each aligned block of 80 rows (0 to 79, 80 to 159, ...) at most 30 rows name the same one
- expert_weight: float32 [2560, 2], P(('sp', 'tp')), may hold values from 0.1 to 1
- gate_proj: bfloat16 [8, 2048, 2048], P('sp', None, 'tp'), may hold values from -0.125 to 0.125
- up_proj: bfloat16 [8, 2048, 2048], P('sp', None, 'tp'), may hold values from -0.125 to 0.125
- down_proj: bfloat16 [8, 2048, 2048], P('sp', 'tp'), may hold values from -0.125 to 0.125
Outputs:
- layer_out: bfloat16 [2560, 2048], P(('sp', 'tp'))
The draws below stay inside these ranges and needn't reach their ends.
Inputs may be any that keep to these rules, and one draw needn't show every extreme that they name: `expert_ids`: each row names 2 different experts. Among the 80 rows of one device no expert is named more than 30 times, and in some device's rows some expert is named exactly 30 times.
All inputs are finite; a program needn't handle non-finite values.
Results may differ from the reference program's by a relative error of at most 0.014.
Values may be sent and summed in bfloat16 or wider, within the bound.
No kernel may reach another device: no remote copies, remote signals or barrier semaphores. Data moves between devices by JAX's collectives and lax.ppermute only.
A program may use at most 128 MiB of HBM per device.

```python
import math
import jax
import jax.numpy as jnp
import numpy as np
from jax import lax

D = 2048
HG = 8
DKS = 64
DKB = 128
VD = 128
FF = 2048
TOPK = 2
TOK_DEV = 320
TOKENS = 2560
TR = 80
EXPERTS = 8
CAP = 30
N_TP = 4


def drawn_pair(key, key_size):
    width = HG * 2 * key_size
    key_query, key_keys = jax.random.split(key, 2)
    query = jnp.clip(1.3 * jax.random.normal(key_query, (TOKENS, width), jnp.float32), -5.2, 5.2)
    keys = jnp.clip(1.3 * jax.random.normal(key_keys, (TOKENS, width), jnp.float32), -5.2, 5.2)
    return (query, keys)


def draw_query_narrow(key, part):
    return drawn_pair(jax.random.fold_in(key, 11), DKS)[0].astype(jnp.bfloat16)


def draw_key_narrow(key, part):
    return drawn_pair(jax.random.fold_in(key, 11), DKS)[1].astype(jnp.bfloat16)


def draw_query_wide(key, part):
    return drawn_pair(jax.random.fold_in(key, 12), DKB)[0].astype(jnp.bfloat16)


def draw_key_wide(key, part):
    return drawn_pair(jax.random.fold_in(key, 12), DKB)[1].astype(jnp.bfloat16)


def shard_levels(key, dims, cuts, least, largest):
    def one(dim, parts):
        draws = jax.random.uniform(jax.random.fold_in(jax.random.fold_in(key, 6), dim), (parts,), jnp.float32, least / len(cuts), largest / len(cuts))
        return jnp.repeat(jnp.exp(draws), dims[dim] // parts).reshape((-1,) + (1,) * (len(dims) - dim - 1))

    loudness = one(*cuts[0])
    for cut in cuts[1:]:
        loudness = loudness * one(*cut)
    return loudness


def routed_block(stream_key, own, number, rows, amount, top, limit, slope):
    order = jax.random.permutation(stream_key, amount)
    crowded, ordinary = portions_of(amount, rows * top, limit, slope, True), portions_of(amount, rows * top, limit, slope, False)
    places = jnp.arange(amount)

    def named(sizes, rotation):
        used = int((sizes > 0).sum())
        fixed = max(1, used // 4)
        passed = fixed + (places - fixed + rotation * (used - fixed)) % max(1, amount - fixed)
        return jnp.zeros((amount,), jnp.int32).at[order[jnp.where(places < fixed, places, passed)]].set(jnp.asarray(sizes, jnp.int32))

    sizes = jnp.where(number % 4 == 0, named(crowded, number // 4), named(ordinary, number - number // 4 - 1))
    mixed = jax.random.permutation(jax.random.fold_in(own, 3), amount)
    giver, sink = mixed[0:amount // 2 * 2:2], mixed[1:amount // 2 * 2:2]
    room = jnp.minimum(sizes[giver] - 1, limit - sizes[sink]) // 2
    room = jnp.where((giver == order[0]) | (sink == order[0]) | (sizes[sink] == 0), 0, jnp.maximum(room, 0))
    passed = jax.random.randint(jax.random.fold_in(own, 4), (amount // 2,), 0, 1 << 20) % (room + 1)
    sizes = sizes.at[giver].add(-passed).at[sink].add(passed)
    items = jnp.searchsorted(jnp.cumsum(sizes), jnp.arange(rows * top), side="right").astype(jnp.int32)
    grid = items.reshape(top, rows).T
    grid = grid[jax.random.permutation(jax.random.fold_in(own, 1), rows)]
    rotation = jax.random.randint(jax.random.fold_in(own, 2), (rows, 1), 0, top)
    return jnp.take_along_axis(grid, (jnp.arange(top)[None, :] + rotation) % top, axis=1)


def portions_of(number_of, total, reach, skew, full):
    portions = [(1 << 20) // math.isqrt(rank ** skew) + 1 for rank in range(1, number_of + 1)]
    largest = reach if full else min(reach, max(-(-total // number_of), total * portions[0] // sum(portions)))
    least = 1 if total - largest >= number_of - 1 else 0
    given, rest = [largest] + [least] * (number_of - 1), total - largest - least * (number_of - 1)
    while rest > 0:
        candidates = [i for i in range(1, number_of) if given[i] < largest] or [i for i in range(1, number_of) if given[i] < reach]
        whole, left = sum([portions[i] for i in candidates]), rest
        for i in candidates:
            more = min(reach - given[i], max(1, left * portions[i] // whole), rest)
            given[i] = given[i] + more
            rest = rest - more
    return np.array(given)


def gaussian(rng, extent, scale, bound, shards=(), kind=jnp.bfloat16):
    result = scale * jax.random.normal(rng, extent, jnp.float32)
    if shards:
        result = result * shard_levels(rng, extent, shards, -0.22, 0.18)
    return jnp.clip(result, -bound, bound).astype(kind)


def setup_inputs(seed: int = 0) -> dict:
    seeds = jax.random.split(jax.random.key(seed), 20)
    residual = gaussian(seeds[0], (TOKENS, D), 1.0, 6.0, ((0, 32),))
    query_narrow = draw_query_narrow(jax.random.fold_in(seeds[19], 71), 0)
    key_narrow = draw_key_narrow(jax.random.fold_in(seeds[19], 71), 0)
    value_narrow = gaussian(seeds[3], (TOKENS, HG * VD), 1.0, 6.0, ((0, 8), (1, 4)))
    query_wide = draw_query_wide(jax.random.fold_in(seeds[19], 71), 0)
    key_wide = draw_key_wide(jax.random.fold_in(seeds[19], 71), 0)
    value_wide = gaussian(seeds[6], (TOKENS, HG * VD), 1.0, 6.0, ((0, 8), (1, 4)))
    subtract_narrow = jnp.clip(0.3 + 0.5 * jax.random.uniform(seeds[7], (HG,), jnp.float32) ** shard_levels(seeds[7], (HG,), ((0, 4),), -0.2, 0.2), 0.3, 0.8)
    subtract_wide = jnp.clip(0.3 + 0.5 * jax.random.uniform(seeds[8], (HG,), jnp.float32) ** shard_levels(seeds[8], (HG,), ((0, 4),), -0.2, 0.2), 0.3, 0.8)
    head_gain = jnp.clip(1.0 + 0.18 * jax.random.normal(seeds[9], (VD,), jnp.float32), 0.1, 1.9)
    out_narrow = gaussian(seeds[10], (HG * VD, D), (2 * HG * VD) ** -0.5, 0.125)
    out_wide = gaussian(seeds[11], (HG * VD, D), (2 * HG * VD) ** -0.5, 0.125)
    norm1_gain = jnp.clip(1.0 + 0.18 * jax.random.normal(seeds[12], (D,), jnp.float32), 0.1, 1.9)
    norm2_gain = jnp.clip(1.0 + 0.18 * jax.random.normal(seeds[13], (D,), jnp.float32), 0.1, 1.9)
    expert_ids_keys = jax.random.split(jax.random.fold_in(seeds[14], 1), TOKENS // TR)
    expert_ids_turns = jax.random.permutation(jax.random.fold_in(seeds[14], 3), TOKENS // TR)
    expert_ids = jax.vmap(lambda own, number: routed_block(jax.random.fold_in(seeds[14], 2), own, number, TR, EXPERTS, TOPK, CAP, 2))(expert_ids_keys, expert_ids_turns).reshape((TOKENS, TOPK))
    expert_weight = jnp.clip(0.1 + 0.9 * jax.random.uniform(seeds[15], (TOKENS, TOPK), jnp.float32) ** shard_levels(seeds[15], (TOKENS, TOPK), ((0, 32),), -0.2, 0.2), 0.1, 1.0)
    gate_proj = gaussian(seeds[16], (EXPERTS, D, FF), D ** -0.5, 0.125, ((0, 8), (2, 4)))
    up_proj = gaussian(seeds[17], (EXPERTS, D, FF), D ** -0.5, 0.125, ((0, 8), (2, 4)))
    down_proj = gaussian(seeds[18], (EXPERTS, FF, D), FF ** -0.5, 0.125, ((0, 8), (1, 4)))
    return {"residual": residual, "query_narrow": query_narrow, "key_narrow": key_narrow, "value_narrow": value_narrow, "query_wide": query_wide, "key_wide": key_wide, "value_wide": value_wide, "subtract_narrow": subtract_narrow, "subtract_wide": subtract_wide, "head_gain": head_gain, "out_narrow": out_narrow, "out_wide": out_wide, "norm1_gain": norm1_gain, "norm2_gain": norm2_gain, "expert_ids": expert_ids, "expert_weight": expert_weight, "gate_proj": gate_proj, "up_proj": up_proj, "down_proj": down_proj}


residual_scale = 2.0 ** 0.5

def layer_norm(values, gain):
    center = lax.optimization_barrier(jnp.mean(values, -1, keepdims=True))
    spread = lax.optimization_barrier(jnp.mean(jnp.square(values - center), -1, keepdims=True))
    return (values - center) * lax.rsqrt(spread + 1e-05) * gain

def attend_block(block, keys, values, subtract, head_gain, key_size):
    scores = jnp.einsum('qhmd,khmd->hmqk', block.astype(jnp.float32), keys.astype(jnp.float32)) * key_size ** (-0.5)
    rowtop = lax.optimization_barrier(jnp.max(scores, -1, keepdims=True))
    expo = jnp.exp(scores - rowtop)
    total = lax.optimization_barrier(jnp.sum(expo, -1))
    weights = expo.astype(jnp.bfloat16)
    mapped = jnp.einsum('hmqk,khe->hmqe', weights.astype(jnp.float32), values.astype(jnp.float32)) / total[..., None]
    diff = mapped[:, 0] - subtract[:, None, None] * mapped[:, 1]
    normed = diff * lax.rsqrt(lax.optimization_barrier(jnp.mean(diff * diff, -1, keepdims=True)) + 1e-06) * head_gain
    return jnp.transpose(normed, (1, 0, 2)).reshape(block.shape[0], -1).astype(jnp.bfloat16)

def attend(query, keys, values, subtract, head_gain):
    tokens = query.shape[0]
    head_count = subtract.shape[0]
    key_size = query.shape[1] // (2 * head_count)
    queries = query.reshape(tokens, head_count, 2, key_size)
    key_rows = keys.reshape(tokens, head_count, 2, key_size)
    value_rows = values.reshape(tokens, head_count, -1)
    span = math.gcd(tokens, 256)
    blocks = queries.reshape(tokens // span, span, head_count, 2, key_size)

    def one_block(block):
        return attend_block(block, key_rows, value_rows, subtract, head_gain, key_size)
    return lax.map(one_block, blocks).reshape(tokens, -1)

def experts_output(hidden, expert_ids, expert_weight, gate_proj, up_proj, down_proj):
    tokens, top_count = expert_ids.shape
    experts = gate_proj.shape[0]
    rows = TOK_DEV // N_TP
    blocks = tokens // rows
    capacity = max(2, 3 * rows * top_count // (2 * experts))
    ids = expert_ids.reshape(blocks, rows * top_count)
    onehot = (ids[..., None] == jnp.arange(experts, dtype=jnp.int32)).astype(jnp.int32)
    before = jnp.cumsum(onehot, 1) - onehot
    position = lax.optimization_barrier(jnp.sum(before * onehot, -1)).astype(jnp.int32)
    column = jnp.arange(blocks, dtype=jnp.int32)[:, None] * capacity + position
    owner = jnp.repeat(jnp.arange(tokens, dtype=jnp.int32), top_count).reshape(blocks, rows * top_count)
    table = jnp.full((experts, blocks * capacity), tokens, jnp.int32)
    table = table.at[ids.reshape(-1), column.reshape(-1)].set(owner.reshape(-1))
    padded = jnp.concatenate([hidden, jnp.zeros((1, hidden.shape[1]), jnp.bfloat16)], 0)
    width = gate_proj.shape[2] // N_TP

    def one_expert(operands):
        picks, w_gate, w_up, w_down = operands
        taken = padded[picks]
        summed = jnp.zeros((picks.shape[0], hidden.shape[1]), jnp.float32)
        for piece in range(N_TP):
            gate_part = jnp.dot(taken, w_gate[:, piece * width:(piece + 1) * width], preferred_element_type=jnp.float32)
            up_part = jnp.dot(taken, w_up[:, piece * width:(piece + 1) * width], preferred_element_type=jnp.float32)
            inner = (jax.nn.silu(gate_part) * up_part).astype(jnp.bfloat16)
            partial_out = jnp.dot(inner, w_down[piece * width:(piece + 1) * width], preferred_element_type=jnp.float32)
            rounded = lax.optimization_barrier(partial_out.astype(jnp.bfloat16))
            summed = summed + rounded.astype(jnp.float32)
        return summed.astype(jnp.bfloat16)
    results = lax.map(one_expert, (table, gate_proj, up_proj, down_proj))
    flat = results.reshape(experts * blocks * capacity, -1)
    where_rows = (ids * (blocks * capacity) + column).reshape(tokens, top_count)
    gathered = flat[where_rows].astype(jnp.float32)
    return lax.optimization_barrier(jnp.sum(expert_weight[..., None] * gathered, 1))

def reference(residual, query_narrow, key_narrow, value_narrow, query_wide, key_wide, value_wide, subtract_narrow, subtract_wide, head_gain, out_narrow, out_wide, norm1_gain, norm2_gain, expert_ids, expert_weight, gate_proj, up_proj, down_proj):
    attended_narrow = attend(query_narrow, key_narrow, value_narrow, subtract_narrow, head_gain)
    attended_wide = attend(query_wide, key_wide, value_wide, subtract_wide, head_gain)
    mix = jnp.dot(attended_narrow, out_narrow, preferred_element_type=jnp.float32) + jnp.dot(attended_wide, out_wide, preferred_element_type=jnp.float32)
    hidden = layer_norm(residual_scale * residual.astype(jnp.float32) + mix, norm1_gain).astype(jnp.bfloat16)
    routed = experts_output(hidden, expert_ids, expert_weight, gate_proj, up_proj, down_proj)
    return layer_norm(residual_scale * hidden.astype(jnp.float32) + routed, norm2_gain).astype(jnp.bfloat16)
```

```python
import math

import jax
import jax.numpy as jnp
from jax import lax
from jax.experimental import pallas as pl
from jax.experimental.pallas import tpu as pltpu
from jax.sharding import PartitionSpec as P


residual_scale = 2.0**0.5
log2_e = 1.0 / math.log(2.0)
lanes = 128


def layer_norm(values, gain):
    center = jnp.mean(values, -1, keepdims=True)
    spread = jnp.mean(jnp.square(values - center), -1, keepdims=True)
    return (values - center) * lax.rsqrt(spread + 1e-05) * gain


def swap(value, axis, flip, keep=None):
    count = lax.axis_size(axis)
    pairs = [(i, i ^ flip) for i in range(count) if keep is None or keep(i ^ flip)]
    return lax.ppermute(value, axis, pairs)


def vmem():
    return pl.BlockSpec(memory_space=pltpu.VMEM)


def smem():
    return pl.BlockSpec(memory_space=pltpu.SMEM)


def pack_body(place, qn, kn, vn, qw, kw, vw, *outs):
    rows = qn.shape[0]
    planes = len(outs) // 2
    for k in range(planes):
        head = place[0] ^ k
        one = pl.ds(pl.multiple_of((head >> 1) * lanes, lanes), lanes)
        first = pl.ds(pl.multiple_of((head >> 1) * 2 * lanes, lanes), lanes)
        second = pl.ds(pl.multiple_of((head >> 1) * 2 * lanes + lanes, lanes), lanes)
        main, extra = outs[2 * k], outs[2 * k + 1]

        @pl.when((head & 1) == 0)
        def _():
            main[0:rows] = kn[:, one]
            main[rows : 2 * rows] = vn[:, one]
            main[2 * rows : 3 * rows] = qn[:, one]
            extra[...] = jnp.zeros(extra.shape, extra.dtype)

        @pl.when((head & 1) == 1)
        def _():
            main[0:rows] = kw[:, first]
            main[rows : 2 * rows] = vw[:, one]
            main[2 * rows : 3 * rows] = qw[:, first]
            extra[0:rows] = kw[:, second]
            extra[rows : 2 * rows] = qw[:, second]


def pack_heads(place, planes, arrays):
    rows = arrays[0].shape[0]
    shapes = []
    for _ in range(planes):
        shapes += [
            jax.ShapeDtypeStruct((3 * rows, lanes), jnp.bfloat16),
            jax.ShapeDtypeStruct((2 * rows, lanes), jnp.bfloat16),
        ]
    return pl.pallas_call(
        pack_body,
        out_shape=shapes,
        in_specs=[smem()] + [vmem()] * 6,
        out_specs=[vmem()] * len(shapes),
        name="pack_heads",
    )(place, *arrays)


def attend_body(place, sub_n, sub_w, gain, *refs):
    planes = (len(refs) - 6) // 4
    mains, extras = refs[:planes], refs[planes : 2 * planes]
    far_mains, far_extras = refs[2 * planes : 3 * planes], refs[3 * planes : 4 * planes]
    out, keys0, keys1, vals, queries0, queries1 = refs[4 * planes :]
    rows = extras[0].shape[0] // 2
    block = out.shape[0]
    head = place[0]
    wide = (head & 1) == 1

    @pl.when(pl.program_id(0) == 0)
    def _():
        low = lax.broadcasted_iota(jnp.int32, (rows, lanes), 1) < lanes // 2
        zero = jnp.zeros((rows, lanes), jnp.bfloat16)
        for k in range(planes):
            for far in range(2):
                main = far_mains[k] if far else mains[k]
                extra = far_extras[k] if far else extras[k]
                at = (2 * k + far) * rows
                vals[at : at + rows] = main[rows : 2 * rows]
                key = main[0:rows]

                @pl.when(wide)
                def _():
                    keys0[at : at + rows] = key
                    keys1[at : at + rows] = extra[0:rows]

                @pl.when(jnp.logical_not(wide))
                def _():
                    keys0[at : at + rows] = jnp.where(low, key, zero)
                    keys1[at : at + rows] = jnp.where(low, zero, key)

            query = mains[k][2 * rows : 3 * rows]
            queries0[k * rows : (k + 1) * rows] = query

            @pl.when(wide)
            def _():
                queries1[k * rows : (k + 1) * rows] = extras[k][rows : 2 * rows]

            @pl.when(jnp.logical_not(wide))
            def _():
                queries1[k * rows : (k + 1) * rows] = query

    scale = jnp.where(wide, float(lanes) ** -0.5, float(lanes // 2) ** -0.5) * log2_e
    span = pl.ds(pl.multiple_of(pl.program_id(0) * block, block), block)

    def mapped(queries, keys):
        scores = lax.dot_general(
            queries[span], keys[...], (((1,), (1,)), ((), ())), preferred_element_type=jnp.float32
        )
        top = jnp.max(scores, -1, keepdims=True)
        expo = jnp.exp2((scores - top) * scale)
        total = jnp.sum(expo, -1, keepdims=True)
        summed = jnp.dot(
            expo.astype(jnp.bfloat16), vals[...], preferred_element_type=jnp.float32
        )
        return summed / total

    subtract = jnp.where(wide, sub_w[head >> 1], sub_n[head >> 1])
    diff = mapped(queries0, keys0) - subtract * mapped(queries1, keys1)
    normed = diff * lax.rsqrt(jnp.mean(diff * diff, -1, keepdims=True) + 1e-06) * gain[...]
    out[...] = normed.astype(jnp.bfloat16)


def attend_heads(place, sub_n, sub_w, gain, mains, extras, far_mains, far_extras):
    planes = len(mains)
    rows = extras[0].shape[0] // 2
    total = planes * rows
    block = math.gcd(total, 128)
    flat = [*mains, *extras, *far_mains, *far_extras]
    return pl.pallas_call(
        attend_body,
        out_shape=jax.ShapeDtypeStruct((total, lanes), jnp.bfloat16),
        grid=(total // block,),
        in_specs=[smem()] * 3 + [vmem()] * (1 + len(flat)),
        out_specs=pl.BlockSpec((block, lanes), lambda i: (i, 0)),
        scratch_shapes=[pltpu.VMEM((2 * total, lanes), jnp.bfloat16)] * 3
        + [pltpu.VMEM((total, lanes), jnp.bfloat16)] * 2,
        name="attend_heads",
    )(place, sub_n, sub_w, gain, *flat)


def mixer_body(place, residual, out_n, out_w, gain, table, *refs):
    groups = len(refs) - 4
    parts = refs[:groups]
    hidden, outgoing, side_n, side_w = refs[groups:]
    planes = parts[0].shape[0]
    per = planes // 2
    for flip in range(groups):
        for k in range(planes):
            head = place[0] ^ k
            at = ((place[1] ^ flip) * per + (head >> 1)) * lanes
            columns = pl.ds(pl.multiple_of(at, lanes), lanes)

            @pl.when((head & 1) == 0)
            def _():
                side_n[:, columns] = parts[flip][k]

            @pl.when((head & 1) == 1)
            def _():
                side_w[:, columns] = parts[flip][k]

    mix = jnp.dot(side_n[...], out_n[...], preferred_element_type=jnp.float32) + jnp.dot(
        side_w[...], out_w[...], preferred_element_type=jnp.float32
    )
    values = layer_norm(residual_scale * residual[...].astype(jnp.float32) + mix, gain[...])
    hidden[...] = values.astype(jnp.bfloat16)
    outgoing[...] = jnp.dot(
        table[...], hidden[...], preferred_element_type=jnp.float32
    ).astype(jnp.bfloat16)


def mixer(place, residual, out_n, out_w, gain, table, parts):
    rows, width = residual.shape
    side = pltpu.VMEM((rows, out_n.shape[0]), jnp.bfloat16)
    return pl.pallas_call(
        mixer_body,
        out_shape=[
            jax.ShapeDtypeStruct((rows, width), jnp.bfloat16),
            jax.ShapeDtypeStruct((table.shape[0], width), jnp.bfloat16),
        ],
        in_specs=[smem()] + [vmem()] * (5 + len(parts)),
        out_specs=[vmem()] * 2,
        scratch_shapes=[side, side],
        name="mixer",
    )(place, residual, out_n, out_w, gain, table, *parts)


def expert_body(taken, mate, w_gate, w_up, w_down, own_out, mate_out):
    for source, target in ((mate, mate_out), (taken, own_out)):
        rows = source[...]
        gate_part = jnp.dot(rows, w_gate[...], preferred_element_type=jnp.float32)
        up_part = jnp.dot(rows, w_up[...], preferred_element_type=jnp.float32)
        inner = (gate_part * jax.nn.sigmoid(gate_part) * up_part).astype(jnp.bfloat16)
        target[...] = jnp.dot(inner, w_down[...], preferred_element_type=jnp.float32).astype(
            jnp.bfloat16
        )


def expert(taken, mate, w_gate, w_up, w_down):
    return pl.pallas_call(
        expert_body,
        out_shape=[jax.ShapeDtypeStruct(taken.shape, jnp.bfloat16)] * 2,
        in_specs=[vmem()] * 5,
        out_specs=[vmem()] * 2,
        name="expert",
    )(taken, mate, w_gate, w_up, w_down)


def combine_body(hidden, gain, weight, picks, *refs):
    back, out = refs[:-1], refs[-1]
    rows = hidden.shape[0]
    returned = jnp.concatenate([piece[...] for piece in back], 0)
    picked = jnp.dot(picks[...], returned, preferred_element_type=jnp.float32)
    routed = residual_scale * hidden[...].astype(jnp.float32)
    mixed = weight[:, 0:1] * picked[0:rows]
    for choice in range(1, weight.shape[1]):
        mixed = mixed + weight[:, choice : choice + 1] * picked[choice * rows : (choice + 1) * rows]
    out[...] = layer_norm(routed + mixed, gain[...]).astype(jnp.bfloat16)


def combine(hidden, gain, weight, picks, back):
    return pl.pallas_call(
        combine_body,
        out_shape=jax.ShapeDtypeStruct(hidden.shape, jnp.bfloat16),
        in_specs=[vmem()] * (4 + len(back)),
        out_specs=vmem(),
        name="combine",
    )(hidden, gain, weight, picks, *back)


def add_rounded(one, other):
    return (one.astype(jnp.float32) + other.astype(jnp.float32)).astype(jnp.bfloat16)


def near_square(count):
    size = 1
    while (2 * size) ** 2 <= count:
        size = 2 * size
    return size


def paired_device(
    residual,
    query_narrow,
    key_narrow,
    value_narrow,
    query_wide,
    key_wide,
    value_wide,
    subtract_narrow,
    subtract_wide,
    head_gain,
    out_narrow,
    out_wide,
    norm1_gain,
    norm2_gain,
    expert_ids,
    expert_weight,
    gate_proj,
    up_proj,
    down_proj,
):
    experts = lax.axis_size("sp")
    groups = lax.axis_size("tp")
    across = near_square(experts)
    planes = experts // across
    seat = lax.axis_index("sp")
    plane = seat // across
    column = lax.axis_index("tp")
    place = jnp.stack([plane, column]).astype(jnp.int32)
    local_rows, top_count = expert_ids.shape

    capacity = max(2, 3 * local_rows * top_count // (2 * experts))
    depth = -(-capacity // 16) * 16
    flat_ids = expert_ids.reshape(-1)
    onehot = (flat_ids[:, None] == jnp.arange(experts, dtype=jnp.int32)[None, :]).astype(jnp.int32)
    before = jnp.cumsum(onehot, 0) - onehot
    position = jnp.sum(before * onehot, 1)
    slots = ((flat_ids ^ seat) * depth + position).reshape(local_rows, top_count)
    wanted = slots.T.reshape(-1)
    picks = (wanted[:, None] == jnp.arange(experts * depth, dtype=jnp.int32)[None, :]).astype(
        jnp.bfloat16
    )
    table = jnp.any(
        jnp.arange(experts * depth, dtype=jnp.int32)[:, None, None] == slots[None], -1
    ).astype(jnp.bfloat16)

    packed = pack_heads(
        place,
        planes,
        (query_narrow, key_narrow, value_narrow, query_wide, key_wide, value_wide),
    )
    rows = query_narrow.shape[0]
    mains, extras = [packed[0]], [packed[1]]
    for k in range(1, planes):
        mains.append(swap(packed[2 * k], "sp", k * across))
        extras.append(
            swap(packed[2 * k + 1], "sp", k * across, lambda to: (to // across) % 2 == 1)
        )
    far_mains = [swap(main[: 2 * rows], "sp", 1) for main in mains]
    far_extras = [
        swap(extra[:rows], "sp", 1, lambda to: (to // across) % 2 == 1) for extra in extras
    ]
    attended = attend_heads(
        place,
        subtract_narrow,
        subtract_wide,
        head_gain[None, :],
        mains,
        extras,
        far_mains,
        far_extras,
    )
    pieces = [attended[:rows]]
    for k in range(1, planes):
        pieces.append(swap(attended[k * rows : (k + 1) * rows], "sp", k * across))
    heads = jnp.stack(pieces, 0)
    parts = []
    for flip in range(groups):
        part = lax.dynamic_slice_in_dim(heads, (column ^ flip) * local_rows, local_rows, 1)
        parts.append(swap(part, "tp", flip) if flip else part)
    hidden, outgoing = mixer(
        place, residual, out_narrow, out_wide, norm1_gain[None, :], table, parts
    )

    half = experts // 2
    arrived = {0: outgoing[:depth]}
    for k in list(range(half, experts)) + list(range(1, half)):
        arrived[k] = swap(outgoing[k * depth : (k + 1) * depth], "sp", k)
    finals = {}
    for start in (0, half):
        mine = jnp.concatenate([arrived[k] for k in range(start, start + half)], 0)
        both = jnp.concatenate([mine, swap(mine, "tp", 2)], 0)
        own_part, mate_part = expert(
            both, swap(both, "tp", 1), gate_proj[0], up_proj[0], down_proj[0]
        )
        paired = add_rounded(own_part, swap(mate_part, "tp", 1))
        share = half * depth
        finals[start] = add_rounded(paired[:share], swap(paired[share:], "tp", 2))
    back = []
    for k in range(experts):
        start = 0 if k < half else half
        piece = finals[start][(k - start) * depth : (k - start + 1) * depth]
        back.append(swap(piece, "sp", k) if k else piece)
    return combine(hidden, norm2_gain[None, :], expert_weight, picks, back)


def block_take(shards, shard_rows):
    take = shards
    for count in range(shards, 0, -1):
        if shards % count == 0 and count * shard_rows >= 512:
            take = count
    return take


def start_carry(head_count, tok_rows, value_size):
    return (
        jnp.full((head_count, 2, tok_rows), -1e30, jnp.float32),
        jnp.zeros((head_count, 2, tok_rows), jnp.float32),
        jnp.zeros((head_count, 2, tok_rows, value_size), jnp.float32),
    )


def absorb_keys(carry, queries, key_piece, value_piece, shard_rows):
    head_count = queries.shape[1]
    key_size = queries.shape[3]
    shards = key_piece.shape[0] // shard_rows
    take = block_take(shards, shard_rows)
    span = take * shard_rows

    def one_block(step_index, state):
        rowtop, total, summed = state
        key_block = lax.dynamic_slice_in_dim(key_piece, step_index * span, span, 0).reshape(
            span, head_count, 2, key_size
        )
        value_block = lax.dynamic_slice_in_dim(value_piece, step_index * span, span, 0).reshape(
            span, head_count, -1
        )
        scores = jnp.einsum(
            "qhmd,khmd->hmqk", queries, key_block, preferred_element_type=jnp.float32
        ) * key_size ** (-0.5)
        newtop = jnp.maximum(rowtop, jnp.max(scores, -1))
        shrink = jnp.exp(rowtop - newtop)
        expo = jnp.exp(scores - newtop[..., None])
        total = total * shrink + jnp.sum(expo, -1)
        summed = summed * shrink[..., None] + jnp.einsum(
            "hmqk,khe->hmqe",
            expo.astype(jnp.bfloat16),
            value_block,
            preferred_element_type=jnp.float32,
        )
        return (newtop, total, summed)

    return lax.fori_loop(0, shards // take, one_block, carry)


def finish_heads(carry, subtract, head_gain):
    rowtop, total, summed = carry
    mapped = summed / total[..., None]
    diff = mapped[:, 0] - subtract[:, None, None] * mapped[:, 1]
    normed = diff * lax.rsqrt(jnp.mean(diff * diff, -1, keepdims=True) + 1e-06) * head_gain
    return jnp.transpose(normed, (1, 0, 2)).reshape(diff.shape[1], -1).astype(jnp.bfloat16)


def on_device(
    residual,
    query_narrow,
    key_narrow,
    value_narrow,
    query_wide,
    key_wide,
    value_wide,
    subtract_narrow,
    subtract_wide,
    head_gain,
    out_narrow,
    out_wide,
    norm1_gain,
    norm2_gain,
    expert_ids,
    expert_weight,
    gate_proj,
    up_proj,
    down_proj,
):
    tok_rows = query_narrow.shape[0]
    head_count = subtract_narrow.shape[0]
    value_size = head_gain.shape[0]
    narrow_queries = query_narrow.reshape(tok_rows, head_count, 2, -1)
    wide_queries = query_wide.reshape(tok_rows, head_count, 2, -1)
    narrow_start = start_carry(head_count, tok_rows, value_size)
    wide_start = start_carry(head_count, tok_rows, value_size)
    narrow_state = absorb_keys(
        narrow_start,
        narrow_queries,
        lax.all_gather(key_narrow, "sp", axis=0, tiled=True),
        lax.all_gather(value_narrow, "sp", axis=0, tiled=True),
        tok_rows,
    )
    wide_state = absorb_keys(
        wide_start,
        wide_queries,
        lax.all_gather(key_wide, "sp", axis=0, tiled=True),
        lax.all_gather(value_wide, "sp", axis=0, tiled=True),
        tok_rows,
    )
    attended_narrow = finish_heads(narrow_state, subtract_narrow, head_gain)
    attended_wide = finish_heads(wide_state, subtract_wide, head_gain)
    full_narrow, full_wide = (
        lax.all_to_all(attended_narrow, "tp", split_axis=0, concat_axis=1, tiled=True),
        lax.all_to_all(attended_wide, "tp", split_axis=0, concat_axis=1, tiled=True),
    )
    mix = jnp.dot(full_narrow, out_narrow, preferred_element_type=jnp.float32) + jnp.dot(
        full_wide, out_wide, preferred_element_type=jnp.float32
    )
    hidden = layer_norm(residual_scale * residual.astype(jnp.float32) + mix, norm1_gain).astype(
        jnp.bfloat16
    )
    local_rows, top_count = expert_ids.shape
    experts = lax.axis_size("sp")
    capacity = max(2, 3 * local_rows * top_count // (2 * experts))
    flat_ids = expert_ids.reshape(-1)
    onehot = (flat_ids[:, None] == jnp.arange(experts, dtype=jnp.int32)[None, :]).astype(jnp.int32)
    before = jnp.cumsum(onehot, 0) - onehot
    position = jnp.sum(before * onehot, 1)
    slots = (flat_ids * capacity + position).reshape(local_rows, top_count)
    dispatch_table = jnp.any(
        jnp.arange(experts * capacity, dtype=jnp.int32)[:, None, None] == slots[None], -1
    ).astype(jnp.bfloat16)
    outgoing = jnp.dot(dispatch_table, hidden, preferred_element_type=jnp.float32).astype(
        jnp.bfloat16
    )
    outgoing = outgoing.reshape(experts, capacity, -1)
    gathered = lax.all_gather(
        lax.all_to_all(outgoing, "sp", split_axis=0, concat_axis=0, tiled=True),
        "tp",
        axis=1,
        tiled=True,
    )
    flat_rows = gathered.reshape(-1, gathered.shape[2])
    gate_part = jnp.dot(flat_rows, gate_proj[0], preferred_element_type=jnp.float32)
    up_part = jnp.dot(flat_rows, up_proj[0], preferred_element_type=jnp.float32)
    inner = (jax.nn.silu(gate_part) * up_part).astype(jnp.bfloat16)
    partial_out = jnp.dot(inner, down_proj[0], preferred_element_type=jnp.float32).reshape(
        gathered.shape
    )
    summed = lax.psum_scatter(
        partial_out.astype(jnp.bfloat16), "tp", scatter_dimension=1, tiled=True
    )
    returned = lax.all_to_all(summed, "sp", split_axis=0, concat_axis=0, tiled=True)
    returned_flat = returned.reshape(experts * capacity, -1)
    picked = returned_flat[slots].astype(jnp.float32)
    routed = jnp.sum(expert_weight[..., None] * picked, 1)
    return layer_norm(residual_scale * hidden.astype(jnp.float32) + routed, norm2_gain).astype(
        jnp.bfloat16
    )


def solution(mesh):
    placed = (
        P(("sp", "tp"), None),
        P("sp", "tp"),
        P("sp", "tp"),
        P("sp", "tp"),
        P("sp", "tp"),
        P("sp", "tp"),
        P("sp", "tp"),
        P("tp"),
        P("tp"),
        P(),
        P(),
        P(),
        P(),
        P(),
        P(("sp", "tp"), None),
        P(("sp", "tp"), None),
        P("sp", None, "tp"),
        P("sp", None, "tp"),
        P("sp", "tp", None),
    )
    experts, groups = mesh.shape["sp"], mesh.shape["tp"]
    planes = experts // near_square(experts)

    def layer(*arrays):
        paired = (
            near_square(experts) == 2
            and groups == 4
            and experts & (experts - 1) == 0
            and arrays[16].shape[0] == experts
            and arrays[7].shape[0] + arrays[8].shape[0] == groups * planes
            and arrays[9].shape[0] == lanes
            and arrays[1].shape[1] == arrays[7].shape[0] * lanes
            and arrays[4].shape[1] == arrays[8].shape[0] * 2 * lanes
            and arrays[0].shape[0] % (16 * experts * groups) == 0
        )
        return place(paired_device if paired else on_device)(*arrays)

    def place(body):
        return jax.shard_map(
            body, mesh=mesh, in_specs=placed, out_specs=P(("sp", "tp"), None), check_vma=False
        )

    return layer
```
